512 devices in a mesh: ep: 128 (over z, x, core), tp: 4 (over y).
Axes of the slice: x: 4, y: 4, z: 16, core: 2. Of those that a mesh axis runs over, the one named last changes fastest.
Arguments:
- tokens: bfloat16 [16384, 4096], P('ep', 'tp'), may hold values from -6 to 6
- norm_gain: float32 [4096], replicated, may hold values from 0.1 to 1.9
- expert_ids: int32 [16384, 2], P('ep'), may hold values from 0 to 127, all different within a row; in each aligned block of 128 rows (0 to 127, 128 to 255, ...) at most 3 rows name the same one
- expert_gates: float32 [16384, 2], P('ep'), may hold values from 0.2 to 1
- gate_proj: bfloat16 [128, 4096, 512], P('ep', None, 'tp'), may hold values from -0.09375 to 0.09375
- up_proj: bfloat16 [128, 4096, 512], P('ep', None, 'tp'), may hold values from -0.09375 to 0.09375
- down_proj: bfloat16 [128, 512, 4096], P('ep', None, 'tp'), may hold values from -0.25 to 0.25
- shared_gate: bfloat16 [4096, 512], P('ep', 'tp'), may hold values from -0.09375 to 0.09375
- shared_up: bfloat16 [4096, 512], P('ep', 'tp'), may hold values from -0.09375 to 0.09375
- shared_down: bfloat16 [512, 4096], P(None, 'tp'), may hold values from -0.25 to 0.25
Outputs:
- mixed: bfloat16 [16384, 4096], P('ep', 'tp')
The draws below stay inside these ranges and needn't reach their ends.
Inputs may be any that keep to these rules, and one draw needn't show every extreme that they name: `expert_ids`: each row names 2 distinct experts. Among the 128 rows of one index of ep (aligned blocks) no expert is named by more than 3 rows, a bound that some block reaches.
All inputs are finite; a program needn't handle non-finite values.
Results may differ from the reference program's by a relative error of at most 0.0067.
Values may be sent and summed in bfloat16 or wider, within the bound.
A program may use at most 64 MiB of HBM per device.

```python
import math
import jax
import jax.numpy as jnp
import numpy as np
from jax import lax

D = 4096
EXPERT_DIM = 512
SHARED = 512
TOP = 2
TOK_DEV = 128
EXPERTS = 128
CAP = 3
TOKENS = 16384
N_EP = 128


def block_scale(stream_key, shape, shards, least, high):
    level = 1.0
    for axis_at, shards_of in shards:
        draws = jax.random.uniform(jax.random.fold_in(jax.random.fold_in(stream_key, 6), axis_at), (shards_of,), jnp.float32, least / len(shards), high / len(shards))
        level = level * jnp.repeat(jnp.exp(draws), shape[axis_at] // shards_of).reshape((-1,) + (1,) * (len(shape) - 1 - axis_at))
    return level


def routed_block(stream_key, own, number, rows, number_of, top, bound, lean):
    order = jax.random.permutation(stream_key, number_of)
    packed, usual = portions_of(number_of, rows * top, bound, lean, True), portions_of(number_of, rows * top, bound, lean, False)
    places = jnp.arange(number_of)

    def named(lengths, turn):
        used = int((lengths > 0).sum())
        fixed = max(1, used // 4)
        shifted = fixed + (places - fixed + turn * (used - fixed)) % max(1, number_of - fixed)
        return jnp.zeros((number_of,), jnp.int32).at[order[jnp.where(places < fixed, places, shifted)]].set(jnp.asarray(lengths, jnp.int32))

    lengths = jnp.where(number % 4 == 0, named(packed, number // 4), named(usual, number - number // 4 - 1))
    mixed = jax.random.permutation(jax.random.fold_in(own, 3), number_of)
    source_of, taker = mixed[0:number_of // 2 * 2:2], mixed[1:number_of // 2 * 2:2]
    room = jnp.minimum(lengths[source_of] - 1, bound - lengths[taker]) // 2
    room = jnp.where((source_of == order[0]) | (taker == order[0]) | (lengths[taker] == 0), 0, jnp.maximum(room, 0))
    shifted = jax.random.randint(jax.random.fold_in(own, 4), (number_of // 2,), 0, 1 << 20) % (room + 1)
    lengths = lengths.at[source_of].add(-shifted).at[taker].add(shifted)
    items = jnp.searchsorted(jnp.cumsum(lengths), jnp.arange(rows * top), side="right").astype(jnp.int32)
    listing = items.reshape(top, rows).T
    listing = listing[jax.random.permutation(jax.random.fold_in(own, 1), rows)]
    turn = jax.random.randint(jax.random.fold_in(own, 2), (rows, 1), 0, top)
    return jnp.take_along_axis(listing, (jnp.arange(top)[None, :] + turn) % top, axis=1)


def portions_of(amount, total, bound, slope, full):
    weights = [(1 << 20) // math.isqrt(rank ** slope) + 1 for rank in range(1, amount + 1)]
    largest = bound if full else min(bound, max(-(-total // amount), total * weights[0] // sum(weights)))
    least = 1 if total - largest >= amount - 1 else 0
    given, rest = [largest] + [least] * (amount - 1), total - largest - least * (amount - 1)
    while rest > 0:
        movable = [i for i in range(1, amount) if given[i] < largest] or [i for i in range(1, amount) if given[i] < bound]
        whole, budget = sum([weights[i] for i in movable]), rest
        for i in movable:
            extra = min(bound - given[i], max(1, budget * weights[i] // whole), rest)
            given[i] = given[i] + extra
            rest = rest - extra
    return np.array(given)


def scatter_about(own_key, shape, deviation, most, shards=(), held_as=jnp.bfloat16):
    loudness = block_scale(own_key, shape, shards, -0.22, 0.18) if shards else 1.0
    drawn = jax.random.normal(own_key, shape, jnp.float32) * deviation * loudness
    return jnp.minimum(jnp.maximum(drawn, -most), most).astype(held_as)


def setup_inputs(seed: int = 0) -> dict:
    seeds = jax.random.split(jax.random.key(seed), 11)
    tokens = scatter_about(seeds[0], (TOKENS, D), 1.0, 6.0, ((0, 128), (1, 4)))
    norm_gain = jnp.clip(1.0 + 0.18 * jax.random.normal(seeds[1], (D,), jnp.float32), 0.1, 1.9)
    expert_ids_keys = jax.random.split(jax.random.fold_in(seeds[2], 1), TOKENS // TOK_DEV)
    expert_ids_turns = jax.random.permutation(jax.random.fold_in(seeds[2], 3), TOKENS // TOK_DEV)
    expert_ids = jax.vmap(lambda own, number: routed_block(jax.random.fold_in(seeds[2], 2), own, number, TOK_DEV, EXPERTS, TOP, CAP, 2))(expert_ids_keys, expert_ids_turns).reshape((TOKENS, TOP))
    expert_gates = jnp.clip(jnp.exp(math.log(1.0) - 1.609438 * jax.random.uniform(seeds[3], (TOKENS, TOP), jnp.float32) ** block_scale(seeds[3], (TOKENS, TOP), ((0, 128),), -0.2, 0.2)), 0.2, 1.0)
    gate_proj = scatter_about(seeds[4], (EXPERTS, D, EXPERT_DIM), D ** -0.5, 0.09375, ((0, 128), (2, 4)))
    up_proj = scatter_about(seeds[5], (EXPERTS, D, EXPERT_DIM), D ** -0.5, 0.09375, ((0, 128), (2, 4)))
    down_proj = scatter_about(seeds[6], (EXPERTS, EXPERT_DIM, D), EXPERT_DIM ** -0.5, 0.25, ((0, 128), (2, 4)))
    shared_gate = scatter_about(seeds[7], (D, SHARED), D ** -0.5, 0.09375, ((0, 128), (1, 4)))
    shared_up = scatter_about(seeds[8], (D, SHARED), D ** -0.5, 0.09375, ((0, 128), (1, 4)))
    shared_down = scatter_about(seeds[9], (SHARED, D), SHARED ** -0.5, 0.25, ((1, 4),))
    return dict(tokens=tokens, norm_gain=norm_gain, expert_ids=expert_ids, expert_gates=expert_gates, gate_proj=gate_proj, up_proj=up_proj, down_proj=down_proj, shared_gate=shared_gate, shared_up=shared_up, shared_down=shared_down)


def reference(tokens, norm_gain, expert_ids, expert_gates, gate_proj, up_proj, down_proj, shared_gate, shared_up, shared_down):
    floats = tokens.astype(jnp.float32)
    scale = lax.rsqrt(lax.optimization_barrier(jnp.mean(floats * floats, axis=-1, keepdims=True)) + 1e-06)
    normed = (floats * scale * norm_gain[None, :]).astype(jnp.bfloat16)
    shared_g = jnp.dot(normed, shared_gate, preferred_element_type=jnp.float32)
    shared_u = jnp.dot(normed, shared_up, preferred_element_type=jnp.float32)
    shared_hidden = (jax.nn.silu(shared_g) * shared_u).astype(jnp.bfloat16)
    shared_out = jnp.dot(shared_hidden, shared_down, preferred_element_type=jnp.float32)
    ids = expert_ids.reshape(N_EP, TOK_DEV * TOP)
    onehot = (ids[:, :, None] == jnp.arange(EXPERTS, dtype=jnp.int32)[None, None, :]).astype(jnp.int32)
    slots = lax.optimization_barrier(jnp.sum((jnp.cumsum(onehot, axis=1) - onehot) * onehot, axis=-1)).astype(jnp.int32)
    dest = (ids * CAP + slots).astype(jnp.int32)
    local_tok = jnp.repeat(jnp.arange(TOK_DEV, dtype=jnp.int32), TOP)
    glob = local_tok[None, :] + jnp.arange(N_EP, dtype=jnp.int32)[:, None] * TOK_DEV
    blocks = jnp.broadcast_to(jnp.arange(N_EP, dtype=jnp.int32)[:, None], dest.shape)
    owner = jnp.full((N_EP, EXPERTS * CAP), TOKENS, jnp.int32).at[blocks, dest].set(glob)
    weight = jnp.zeros((N_EP, EXPERTS * CAP), jnp.float32).at[blocks, dest].set(expert_gates.reshape(N_EP, TOK_DEV * TOP))
    owner = owner.reshape(N_EP, EXPERTS, CAP).transpose(1, 0, 2).reshape(EXPERTS, N_EP * CAP)
    weight = weight.reshape(N_EP, EXPERTS, CAP).transpose(1, 0, 2).reshape(EXPERTS, N_EP * CAP)
    padded = jnp.concatenate([normed, jnp.zeros((1, D), jnp.bfloat16)], axis=0)

    def step(total, item):
        rows_idx, rows_weight, w_gate, w_up, w_down = item
        rows = padded[rows_idx]
        g = jnp.dot(rows, w_gate, preferred_element_type=jnp.float32)
        u = jnp.dot(rows, w_up, preferred_element_type=jnp.float32)
        hidden = (jax.nn.silu(g) * u).astype(jnp.bfloat16)
        result = jnp.dot(hidden, w_down, preferred_element_type=jnp.float32).astype(jnp.bfloat16)
        return (total.at[rows_idx].add(rows_weight[:, None] * result.astype(jnp.float32)), None)
    total = jnp.zeros((TOKENS + 1, D), jnp.float32)
    total, _ = lax.scan(step, total, (owner, weight, gate_proj, up_proj, down_proj))
    return (total[:TOKENS] + shared_out).astype(jnp.bfloat16)
```

```python
import jax
import jax.numpy as jnp
from jax import lax
from jax.experimental import pallas as pl
from jax.experimental.pallas import tpu as pltpu
from jax.sharding import Mesh
from jax.sharding import PartitionSpec as P

EP = ("ep_0", "ep_1", "ep_2")


def copy_for_each(value, axis):
    peers = lax.axis_size(axis)
    return lax.all_to_all(
        jnp.broadcast_to(value[None], (peers, *value.shape)), axis, 0, 0, tiled=True
    )


def laid_out(blocks, dim):
    shape = list(blocks.shape[1:])
    shape[dim] *= blocks.shape[0]
    return jnp.moveaxis(blocks, 0, dim).reshape(shape)


def collect(value, axis, dim):
    blocks = copy_for_each(value, axis)
    return laid_out(blocks, dim)


def sent_together(arrays, axis, dim, along):
    both = jnp.concatenate(arrays, axis=along)
    filled, at, outs = (lax.all_gather(both, axis, axis=dim, tiled=True), 0, [])
    for a in arrays:
        outs.append(lax.slice_in_dim(filled, at, at + a.shape[along], axis=along))
        at += a.shape[along]
    return tuple(outs)


def split_up(value, dim, peers):
    before, after = (value.shape[:dim], value.shape[dim + 1 :])
    return jnp.moveaxis(value.reshape(*before, peers, -1, *after), dim, 0)


def turned_blocks(blocks, axes, sequence):
    inside = blocks.shape[1:]
    filled = blocks.reshape(*(lax.axis_size(a) for a in axes), *inside)
    for k in sequence:
        filled = lax.all_to_all(filled, axes[k], k, k, tiled=True)
    return filled.reshape(-1, *inside)


def core_and_chips(value, groups, sequence, split_dim, concat_dim):
    peers = lax.axis_size(groups[0]) * lax.axis_size(groups[1])
    blocks = split_up(value, split_dim, peers)
    return laid_out(turned_blocks(blocks, groups, sequence), concat_dim)


MESH = pl.DeviceIdType.MESH


def exchange_kernel(src, dst, send_sem, recv_sem):
    z, x, c, y = (lax.axis_index(a) for a in ("ep_0", "ep_1", "ep_2", "tp"))
    me = (z * 4 + x) * 2 + c

    def peer(i):
        step = i // 8
        half = (step + 1) // 2
        dz = (8 - half) * (step % 2) + (8 + half) * (1 - step % 2)
        w = i % 8
        return (z + dz) % 16, (x + w // 2) % 4, (c + w % 2) % 2, y

    barrier = pltpu.get_barrier_semaphore()

    def greet(i, _):
        pl.semaphore_signal(barrier, inc=1, device_id=peer(i), device_id_type=MESH)
        return 0

    lax.fori_loop(0, 120, greet, 0)
    lax.fori_loop(121, 128, greet, 0)
    pl.semaphore_wait(barrier, 127)

    def send(i, _):
        p = peer(i)
        pltpu.make_async_remote_copy(
            src_ref=src.at[(p[0] * 4 + p[1]) * 2 + p[2]],
            dst_ref=dst.at[me],
            send_sem=send_sem,
            recv_sem=recv_sem,
            device_id=p,
            device_id_type=MESH,
        ).start()
        return 0

    lax.fori_loop(0, 120, send, 0)
    lax.fori_loop(121, 128, send, 0)
    dst[me] = src[me]
    most = pl.ds(0, 127)
    pltpu.make_async_copy(src.at[most], dst.at[most], recv_sem).wait()
    pltpu.make_async_copy(src.at[most], src.at[most], send_sem).wait()


def exchange(blocks):
    return pl.pallas_call(
        exchange_kernel,
        out_shape=jax.ShapeDtypeStruct(blocks.shape, blocks.dtype),
        in_specs=[pl.BlockSpec(memory_space=pltpu.VMEM)],
        out_specs=pl.BlockSpec(memory_space=pltpu.VMEM),
        scratch_shapes=[pltpu.SemaphoreType.DMA, pltpu.SemaphoreType.DMA],
        compiler_params=pltpu.CompilerParams(collective_id=0, has_side_effects=True),
    )(blocks)


def shards(
    tokens,
    norm_gain,
    expert_ids,
    expert_gates,
    gate_proj,
    up_proj,
    down_proj,
    shared_gate,
    shared_up,
    shared_down,
):
    n_ep = lax.axis_size(EP)
    n_tp = lax.axis_size("tp")
    whole = collect(tokens, "tp", 1)
    tok_rows, width = whole.shape
    quarter = width // n_tp
    floats = whole.astype(jnp.float32)
    scale = lax.rsqrt(jnp.mean(floats * floats, axis=-1, keepdims=True) + 1e-06)
    normed = (floats * scale * norm_gain[None, :]).astype(jnp.bfloat16)
    gate_whole, up_whole = sent_together((shared_gate, shared_up), EP, 0, 1)
    shared_g = jnp.dot(normed, gate_whole, preferred_element_type=jnp.float32)
    shared_u = jnp.dot(normed, up_whole, preferred_element_type=jnp.float32)
    shared_hidden = (jax.nn.silu(shared_g) * shared_u).astype(jnp.bfloat16)
    rows = shared_down
    shared_out = jnp.dot(collect(shared_hidden, "tp", 1), rows, preferred_element_type=jnp.float32)
    exp_dev = gate_proj.shape[0]
    n_exp = exp_dev * n_ep
    top = expert_ids.shape[1]
    cap = 3 * tok_rows * top // (2 * n_exp)
    flat_ids = expert_ids.reshape(tok_rows * top)
    onehot = (flat_ids[:, None] == jnp.arange(n_exp, dtype=jnp.int32)[None, :]).astype(jnp.int32)
    slots = jnp.sum((jnp.cumsum(onehot, axis=0) - onehot) * onehot, axis=-1)
    dest = flat_ids * cap + slots
    local_tok = jnp.repeat(jnp.arange(tok_rows, dtype=jnp.int32), top)
    owner = jnp.full((n_exp * cap,), tok_rows, jnp.int32).at[dest].set(local_tok)
    own_part = lax.dynamic_slice_in_dim(normed, lax.axis_index("tp") * quarter, quarter, 1)
    padded = jnp.concatenate([own_part, jnp.zeros((1, quarter), jnp.bfloat16)], axis=0)
    outgoing = padded[owner].reshape(n_ep, 2, exp_dev * cap * quarter // 2)
    arrived = exchange(outgoing).reshape(n_ep, exp_dev, cap, quarter)
    received = collect(arrived, "tp", 3)
    gate_vals = jnp.einsum(
        "secd,edh->sech", received, gate_proj, preferred_element_type=jnp.float32
    )
    up_vals = jnp.einsum("secd,edh->sech", received, up_proj, preferred_element_type=jnp.float32)
    expert_hidden = (jax.nn.silu(gate_vals) * up_vals).astype(jnp.bfloat16)
    rows = down_proj
    expert_out = jnp.einsum(
        "sech,ehd->secd", collect(expert_hidden, "tp", 3), rows, preferred_element_type=jnp.float32
    ).astype(jnp.bfloat16)
    returned = exchange(expert_out.reshape(n_ep, 2, -1))
    picked = returned.reshape(n_exp * cap, quarter)[dest].reshape(tok_rows, top, quarter)
    routed = jnp.sum(expert_gates[:, :, None] * picked.astype(jnp.float32), axis=1)
    return (routed + shared_out).astype(jnp.bfloat16)


def solution(mesh):
    finer = Mesh(mesh.devices.reshape(16, 4, 2, mesh.shape["tp"]), ("ep_0", "ep_1", "ep_2", "tp"))
    in_specs = (
        P(EP, "tp"),
        P(),
        P(EP, None),
        P(EP, None),
        P(EP, None, "tp"),
        P(EP, None, "tp"),
        P(EP, None, "tp"),
        P(EP, "tp"),
        P(EP, "tp"),
        P(None, "tp"),
    )
    out_specs = P(EP, "tp")
    return jax.shard_map(
        shards, mesh=finer, in_specs=in_specs, out_specs=out_specs, check_vma=False
    )
```

```python
import jax
import jax.numpy as jnp
from jax import lax
from jax.experimental import pallas as pl
from jax.experimental.pallas import tpu as pltpu
from jax.sharding import Mesh
from jax.sharding import PartitionSpec as P

EP = ("ep_0", "ep_1", "ep_2")
MESH = pl.DeviceIdType.MESH
BF16 = jnp.bfloat16
F32 = jnp.float32
PLANES, PER_PLANE, PEERS = 16, 8, 128
BATCHES = 4


def offset_of(i):
    half = (i + 1) // 2
    return (i % 2) * half + (1 - i % 2) * ((PLANES - half) % PLANES)


def dot(a, b):
    return jnp.dot(a, b, preferred_element_type=F32)


def parity(shape, axis):
    return lax.broadcasted_iota(jnp.int32, shape, axis) % 2


def swap_pairs(v):
    n = v.shape[0]
    return jnp.where(
        parity(v.shape, 0) == 0, pltpu.roll(v, n - 1, 0), pltpu.roll(v, 1, 0)
    )


def silu_mul(g, u):
    return g / (1.0 + jnp.exp(-g)) * u


def layer_kernel(
    tokens,
    gain,
    ids,
    ids_t,
    gates,
    gate_hbm,
    up_hbm,
    down_hbm,
    shared_gate,
    shared_up,
    shared_down_hbm,
    out,
    send,
    rows,
    mixed_in,
    hidden,
    give,
    got,
    all_tokens,
    shared_w,
    shared_hidden,
    gate_up,
    down,
    shared_down,
    load_sem,
    send_sem,
    row_sem,
    fwd_send,
    fwd_sem,
    hid_send,
    hid_sem,
    give_send,
    got_sem,
    tok_send,
    tok_sem,
    ring_send,
    ring_sem,
    wx_send,
    wx_sem,
    wc_send,
    wc_sem,
    sh_send,
    sh_sem,
):
    z, x, c, y = (lax.axis_index(a) for a in (*EP, "tp"))
    w = x * 2 + c
    me = z * PER_PLANE + w
    tps = (1, 3, 2)

    def remote(src, dst, ssem, rsem, device):
        return pltpu.make_async_remote_copy(
            src_ref=src,
            dst_ref=dst,
            send_sem=ssem,
            recv_sem=rsem,
            device_id=device,
            device_id_type=MESH,
        )

    def drain(ref, sem):
        pltpu.make_async_copy(ref, ref, sem).wait()

    def ep_peer(dz, k):
        return (z + dz) % PLANES, (x + k // 2) % 4, (c + k % 2) % 2, y

    def tp_peer(d):
        return z, x, c, (y + d) % 4

    def index_of(device):
        return (device[0] * 4 + device[1]) * 2 + device[2]

    barrier = pltpu.get_barrier_semaphore()

    def greet(f, _):
        peer = ep_peer(offset_of(f // PER_PLANE), f % PER_PLANE)
        pl.semaphore_signal(barrier, inc=1, device_id=peer, device_id_type=MESH)
        return 0

    lax.fori_loop(1, PEERS, greet, 0)
    for d in tps:
        pl.semaphore_signal(barrier, inc=1, device_id=tp_peer(d), device_id_type=MESH)

    loads = [
        pltpu.make_async_copy(gate_hbm.at[0], gate_up.at[:, pl.ds(0, 128)], load_sem.at[0]),
        pltpu.make_async_copy(up_hbm.at[0], gate_up.at[:, pl.ds(128, 128)], load_sem.at[1]),
        pltpu.make_async_copy(down_hbm.at[0], down, load_sem.at[2]),
        pltpu.make_async_copy(shared_down_hbm, shared_down, load_sem.at[3]),
    ]
    for load in loads:
        load.start()

    tok = tokens[...]
    expert = lax.broadcasted_iota(jnp.int32, (128, 128), 0)
    lane = lax.broadcasted_iota(jnp.int32, (128, 128), 1)
    first_t, second_t = ids_t[0:1, :], ids_t[1:2, :]
    names0, names1 = (expert == first_t).astype(F32), (expert == second_t).astype(F32)
    before = dot((names0 + names1).astype(BF16), (expert < lane).astype(BF16))
    slot0 = jnp.sum(names0 * before, axis=0, keepdims=True).astype(jnp.int32)
    slot1 = jnp.sum(names1 * before, axis=0, keepdims=True).astype(jnp.int32)

    row = lax.broadcasted_iota(jnp.int32, (256, 128), 0)
    pair0 = jnp.where(slot0 < 2, 2 * first_t + slot0, -1)
    pair1 = jnp.where(slot1 < 2, 2 * second_t + slot1, -1)
    last0 = jnp.where(slot0 == 2, first_t, -1)
    last1 = jnp.where(slot1 == 2, second_t, -1)
    pick_pair = ((row == pair0) | (row == pair1)).astype(BF16)
    pick_last = ((row // 2 == last0) | (row // 2 == last1)).astype(BF16)
    send[:, :, :1024] = dot(pick_pair, tok).astype(BF16).reshape(128, 2, 1024)
    whole = dot(pick_last, tok)
    halves = jnp.where(parity((256, 512), 0) == 0, whole[:, :512], whole[:, 512:])
    send[:, :, 1024:] = halves.astype(BF16).reshape(128, 2, 512)
    rows[y, me] = send[me]
    all_tokens[y] = tok
    shared_w[z, w, :, :128] = shared_gate[...]
    shared_w[z, w, :, 128:] = shared_up[...]

    pl.semaphore_wait(barrier, PEERS - 1 + 3)

    def dispatch(f, _):
        i = f // PER_PLANE
        peer = ep_peer(offset_of(i), f % PER_PLANE)
        remote(send.at[index_of(peer)], rows.at[y, me], send_sem, row_sem.at[i], peer).start()
        return 0

    lax.fori_loop(1, PEERS, dispatch, 0)

    def ring(h, side):
        plane = (z + PLANES - (h - 1)) % PLANES if side == 0 else (z + h - 1) % PLANES
        block = shared_w.at[plane, w]
        peer = ep_peer(1 if side == 0 else PLANES - 1, 0)
        return remote(block, block, ring_send, ring_sem.at[side, h - 1], peer)

    def ring_step(h):
        for side in (0, 1):
            if 1 < h and not (side == 1 and h - 1 > 7):
                ring(h - 1, side).wait_recv()
            if h <= (8, 7)[side]:
                ring(h, side).start()

    ring_step(1)

    def plane_of(i):
        return (z + PLANES - offset_of(i)) % PLANES

    def forward(i):
        group = rows.at[y, pl.ds(plane_of(i) * PER_PLANE, PER_PLANE)]
        if i == 0:
            drain(rows.at[y, pl.ds(0, PER_PLANE - 1)], row_sem.at[0])
        else:
            drain(group, row_sem.at[i])
        for n, d in enumerate(tps):
            remote(group, group, fwd_send, fwd_sem.at[n, i], tp_peer(d)).start()

    even = parity((64, 512), 0) == 0

    def expert_in(b):
        for i in range(4 * b, 4 * b + 4):
            for n in range(3):
                drain(rows.at[0, pl.ds(0, PER_PLANE)], fwd_sem.at[n, i])

        def batch(t):
            parts = [
                rows[t, pl.ds(plane_of(i) * PER_PLANE, PER_PLANE)].reshape(16, 1536)
                for i in range(4 * b, 4 * b + 4)
            ]
            return jnp.concatenate(parts, axis=0)

        square_pair, square_last = jnp.zeros((64, 1), F32), jnp.zeros((64, 1), F32)
        for t in range(4):
            v = batch(t).astype(F32)
            sq = v * v
            square_pair += jnp.sum(sq[:, :1024], axis=1, keepdims=True)
            square_last += jnp.sum(sq[:, 1024:], axis=1, keepdims=True)
        last_wide = jnp.broadcast_to(square_last, (64, 128))
        square_last = (last_wide + swap_pairs(last_wide))[:, :1]
        scale_pair = lax.rsqrt(square_pair / 4096.0 + 1e-06)
        scale_last = lax.rsqrt(square_last / 4096.0 + 1e-06)
        for t in range(4):
            v = batch(t).astype(F32)
            g = gain[t : t + 1, :]
            mixed_in[0:64, t * 1024 : (t + 1) * 1024] = (v[:, :1024] * scale_pair * g).astype(BF16)
            last = v[:, 1024:] * scale_last
            for p in (0, 1):
                mine = even if p == 0 else jnp.logical_not(even)
                part = jnp.where(mine, last * g[:, p * 512 : (p + 1) * 512], 0.0)
                at = t * 1024 + p * 512
                mixed_in[64:128, at : at + 512] = part.astype(BF16)
        both = dot(mixed_in[...], gate_up[...])
        tail = both[64:]
        both = jnp.concatenate([both[:64], tail + swap_pairs(tail)], axis=0)
        hidden[y, b] = silu_mul(both[:, :128], both[:, 128:]).astype(BF16)
        for n, d in enumerate(tps):
            remote(hidden.at[y, b], hidden.at[y, b], hid_send, hid_sem.at[n, b], tp_peer(d)).start()

    def expert_out(b):
        for n in range(3):
            drain(hidden.at[0, 0], hid_sem.at[n, b])
        full = jnp.concatenate([hidden[t, b] for t in range(4)], axis=1)
        res = dot(full, down[...])
        tail = jnp.where(even, res[64:, :512], res[64:, 512:])
        res = jnp.concatenate([res[:64], tail], axis=1).astype(BF16)
        for j in range(4):
            i = 4 * b + j
            plane = plane_of(i)
            give[pl.ds(plane * PER_PLANE, PER_PLANE)] = res[16 * j : 16 * j + 16].reshape(8, 2, 1536)
            for k in range(1 if i == 0 else 0, PER_PLANE):
                peer = ep_peer((PLANES - offset_of(i)) % PLANES, k)
                remote(give.at[index_of(peer)], got.at[me], give_send, got_sem, peer).start()
        if b == 0:
            got[me] = give[me]

    def forwards(b):
        for i in range(4 * b, 4 * b + 4):
            forward(i)
            if i % 2 == 1:
                ring_step(i // 2 + 2)

    forwards(0)
    for load in loads:
        load.wait()
    forwards(1)
    expert_in(0)
    forwards(2)
    expert_out(0)
    expert_in(1)
    forwards(3)
    expert_out(1)
    expert_in(2)

    def columns(dx):
        return shared_w.at[:, ((x + 4 - dx) % 4) * 2 + c]

    def other_core(dx):
        return remote(columns(dx), columns(dx), wc_send, wc_sem.at[dx], ep_peer(0, 1))

    for n in (1, 2, 3):
        remote(columns(0), columns(0), wx_send, wx_sem.at[n - 1], ep_peer(0, 2 * n)).start()
    other_core(0).start()
    expert_in(3)
    expert_out(2)
    for n, d in enumerate(tps):
        remote(all_tokens.at[y], all_tokens.at[y], tok_send, tok_sem.at[n], tp_peer(d)).start()
    expert_out(3)
    for n in (1, 2, 3):
        drain(shared_w.at[:, 0], wx_sem.at[n - 1])
        other_core(n).start()

    for n in range(3):
        drain(all_tokens.at[0], tok_sem.at[n])
    square = jnp.zeros((128, 1), F32)
    for t in range(4):
        v = all_tokens[t].astype(F32)
        square += jnp.sum(v * v, axis=1, keepdims=True)
    scale = lax.rsqrt(square / 4096.0 + 1e-06)
    for t in range(4):
        v = all_tokens[t].astype(F32)
        mixed_in[:, t * 1024 : (t + 1) * 1024] = (v * scale * gain[t : t + 1, :]).astype(BF16)
    for n in range(4):
        drain(shared_w.at[:, 0], wc_sem.at[n])
    both = dot(mixed_in[...], shared_w[...].reshape(4096, 256))
    shared_hidden[y] = silu_mul(both[:, :128], both[:, 128:]).astype(BF16)
    for n, d in enumerate(tps):
        remote(shared_hidden.at[y], shared_hidden.at[y], sh_send, sh_sem.at[n], tp_peer(d)).start()

    token = expert
    first, second = ids[:, 0:1], ids[:, 1:2]
    names0, names1 = (lane == first).astype(F32), (lane == second).astype(F32)
    before = dot((lane < token).astype(BF16), (names0 + names1).astype(BF16))
    slot0 = jnp.sum(names0 * before, axis=1, keepdims=True).astype(jnp.int32)
    slot1 = jnp.sum(names1 * before, axis=1, keepdims=True).astype(jnp.int32)
    col = lax.broadcasted_iota(jnp.int32, (128, 256), 1)

    def weights(at, key0, key1):
        return jnp.where(at == key0, gates[:, 0:1], 0.0) + jnp.where(at == key1, gates[:, 1:2], 0.0)

    def parts_of(v):
        high = v.astype(BF16)
        return high, (v - high.astype(F32)).astype(BF16)

    pair = weights(
        col, jnp.where(slot0 < 2, 2 * first + slot0, -1), jnp.where(slot1 < 2, 2 * second + slot1, -1)
    )
    last = weights(col // 2, jnp.where(slot0 == 2, first, -1), jnp.where(slot1 == 2, second, -1))

    for n in range(3):
        drain(shared_hidden.at[0], sh_sem.at[n])
    full = jnp.concatenate([shared_hidden[t] for t in range(4)], axis=1)
    shared_out = dot(full, shared_down[...])

    drain(got.at[pl.ds(0, PEERS - 1)], got_sem)
    back = got[...].reshape(256, 1536)
    total = shared_out
    for part in parts_of(pair):
        total += dot(part, back[:, :1024])
    sides = []
    for p in (0, 1):
        side = jnp.zeros((128, 512), F32)
        for part in parts_of(jnp.where(col % 2 == p, last, 0.0)):
            side += dot(part, back[:, 1024:])
        sides.append(side)
    out[...] = (total + jnp.concatenate(sides, axis=1)).astype(BF16)

    drain(send.at[pl.ds(0, PEERS - 1)], send_sem)
    drain(rows.at[pl.ds(0, 3)], fwd_send)
    drain(hidden.at[pl.ds(0, 3)], hid_send)
    drain(give.at[pl.ds(0, PEERS - 1)], give_send)
    drain(all_tokens.at[pl.ds(0, 3)], tok_send)
    drain(shared_w.at[pl.ds(0, 15), 0], ring_send)
    drain(shared_w.at[:, pl.ds(0, 3)], wx_send)
    drain(shared_w.at[:, pl.ds(0, 4)], wc_send)
    drain(shared_hidden.at[pl.ds(0, 3)], sh_send)


def shards(
    tokens,
    norm_gain,
    expert_ids,
    expert_gates,
    gate_proj,
    up_proj,
    down_proj,
    shared_gate,
    shared_up,
    shared_down,
):
    vmem, hbm = pl.BlockSpec(memory_space=pltpu.VMEM), pl.BlockSpec(memory_space=pl.ANY)
    dma = pltpu.SemaphoreType.DMA
    return pl.pallas_call(
        layer_kernel,
        out_shape=jax.ShapeDtypeStruct(tokens.shape, BF16),
        in_specs=[vmem, vmem, vmem, vmem, vmem, hbm, hbm, hbm, vmem, vmem, hbm],
        out_specs=vmem,
        scratch_shapes=[
            pltpu.VMEM((128, 2, 1536), BF16),
            pltpu.VMEM((4, 128, 2, 1536), BF16),
            pltpu.VMEM((128, 4096), BF16),
            pltpu.VMEM((4, BATCHES, 128, 128), BF16),
            pltpu.VMEM((128, 2, 1536), BF16),
            pltpu.VMEM((128, 2, 1536), BF16),
            pltpu.VMEM((4, 128, 1024), BF16),
            pltpu.VMEM((16, 8, 32, 256), BF16),
            pltpu.VMEM((4, 128, 128), BF16),
            pltpu.VMEM((4096, 256), BF16),
            pltpu.VMEM((512, 1024), BF16),
            pltpu.VMEM((512, 1024), BF16),
            dma((4,)),
            dma,
            dma((16,)),
            dma,
            dma((3, 16)),
            dma,
            dma((3, BATCHES)),
            dma,
            dma,
            dma,
            dma((3,)),
            dma,
            dma((2, 8)),
            dma,
            dma((3,)),
            dma,
            dma((4,)),
            dma,
            dma((3,)),
        ],
        compiler_params=pltpu.CompilerParams(
            collective_id=0, has_side_effects=True, vmem_limit_bytes=60 * 2**20
        ),
    )(
        tokens,
        norm_gain.reshape(4, 1024),
        expert_ids,
        expert_ids.T,
        expert_gates,
        gate_proj,
        up_proj,
        down_proj,
        shared_gate,
        shared_up,
        shared_down,
    )


def solution(mesh):
    finer = Mesh(mesh.devices.reshape(16, 4, 2, mesh.shape["tp"]), (*EP, "tp"))
    in_specs = (
        P(EP, "tp"),
        P(),
        P(EP, None),
        P(EP, None),
        P(EP, None, "tp"),
        P(EP, None, "tp"),
        P(EP, None, "tp"),
        P(EP, "tp"),
        P(EP, "tp"),
        P(None, "tp"),
    )
    return jax.shard_map(
        shards, mesh=finer, in_specs=in_specs, out_specs=P(EP, "tp"), check_vma=False
    )
```

```python
import jax
import jax.numpy as jnp
from jax import lax
from jax.experimental import pallas as pl
from jax.experimental.pallas import tpu as pltpu
from jax.sharding import Mesh
from jax.sharding import PartitionSpec as P

EP = ("ep_0", "ep_1", "ep_2")
MESH = pl.DeviceIdType.MESH
BF16 = jnp.bfloat16
F32 = jnp.float32
PLANES, PER_PLANE, PEERS = 16, 8, 128
BATCHES = 4
NEAR = 4
LAG = 2
RELAYED = 0


ORDER = (0, 1, 15, 2, 14, 3, 13, 4, 12, 5, 11, 6, 10, 7, 9, 8)
SCHEDULE = (
    "R1", "I8", "F0", "F1", "F2", "F3", "R2", "I12", "F4", "F5", "F6", "F7",
    "R3", "I16", "E0", "F8", "F9", "D0", "F10", "F11", "R4", "E1", "F12", "F13",
    "D1", "F14", "F15", "J0", "E2", "E3", "D2", "T0", "D3", "K0", "X0", "S0",
    "S1",
)


def dot(a, b):
    return jnp.dot(a, b, preferred_element_type=F32)


def parity(shape, axis):
    return lax.broadcasted_iota(jnp.int32, shape, axis) % 2


def swap_pairs(v):
    n = v.shape[0]
    return jnp.where(
        parity(v.shape, 0) == 0, pltpu.roll(v, n - 1, 0), pltpu.roll(v, 1, 0)
    )


def silu_mul(g, u):
    return g / (1.0 + jnp.exp(-g)) * u


def layer_kernel(
    tokens,
    gain,
    ids_t,
    gates_t,
    gate_hbm,
    up_hbm,
    down_hbm,
    shared_gate,
    shared_up,
    shared_down_hbm,
    out,
    send,
    rows,
    mixed_in,
    hidden,
    give,
    got,
    all_tokens,
    shared_w,
    shared_hidden,
    normed,
    gate_up,
    down,
    shared_down,
    load_sem,
    send_sem,
    row_sem,
    fwd_send,
    fwd_sem,
    hid_send,
    hid_sem,
    give_send,
    got_sem,
    tok_send,
    tok_sem,
    ring_send,
    ring_sem,
    jump_sem,
    wx_send,
    wx_sem,
    wc_send,
    wc_sem,
    sh_send,
    sh_sem,
):
    z, x, c, y = (lax.axis_index(a) for a in (*EP, "tp"))
    w = x * 2 + c
    me = z * PER_PLANE + w
    tps = (1, 3, 2)

    def remote(src, dst, ssem, rsem, device):
        return pltpu.make_async_remote_copy(
            src_ref=src,
            dst_ref=dst,
            send_sem=ssem,
            recv_sem=rsem,
            device_id=device,
            device_id_type=MESH,
        )

    def drain(ref, sem):
        pltpu.make_async_copy(ref, ref, sem).wait()

    def ep_peer(dz, k):
        return (z + dz) % PLANES, (x + k // 2) % 4, (c + k % 2) % 2, y

    def tp_peer(d):
        return z, x, c, (y + d) % 4

    def index_of(device):
        return (device[0] * 4 + device[1]) * 2 + device[2]

    barrier = pltpu.get_barrier_semaphore()

    for dz in range(PLANES):
        for k in range(0 if dz else 1, PER_PLANE):
            pl.semaphore_signal(barrier, inc=1, device_id=ep_peer(dz, k), device_id_type=MESH)
    for d in tps:
        pl.semaphore_signal(barrier, inc=1, device_id=tp_peer(d), device_id_type=MESH)

    loads = [
        pltpu.make_async_copy(gate_hbm.at[0], gate_up.at[:, pl.ds(0, 128)], load_sem.at[0]),
        pltpu.make_async_copy(up_hbm.at[0], gate_up.at[:, pl.ds(128, 128)], load_sem.at[1]),
        pltpu.make_async_copy(down_hbm.at[0], down, load_sem.at[2]),
        pltpu.make_async_copy(shared_down_hbm, shared_down, load_sem.at[3]),
    ]
    for load in loads:
        load.start()

    tok = tokens[...]
    expert = lax.broadcasted_iota(jnp.int32, (128, 128), 0)
    lane = lax.broadcasted_iota(jnp.int32, (128, 128), 1)
    first_t, second_t = ids_t[0:1, :], ids_t[1:2, :]
    names0, names1 = (expert == first_t).astype(F32), (expert == second_t).astype(F32)
    before = dot((names0 + names1).astype(BF16), (expert < lane).astype(BF16))
    slot0 = jnp.sum(names0 * before, axis=0, keepdims=True).astype(jnp.int32)
    slot1 = jnp.sum(names1 * before, axis=0, keepdims=True).astype(jnp.int32)

    row = lax.broadcasted_iota(jnp.int32, (256, 128), 0)
    pair0 = jnp.where(slot0 < 2, 2 * first_t + slot0, -1)
    pair1 = jnp.where(slot1 < 2, 2 * second_t + slot1, -1)
    last0 = jnp.where(slot0 == 2, first_t, -1)
    last1 = jnp.where(slot1 == 2, second_t, -1)
    pick_pair = ((row == pair0) | (row == pair1)).astype(BF16)
    pick_last = ((row // 2 == last0) | (row // 2 == last1)).astype(BF16)
    send[:, :, :1024] = dot(pick_pair, tok).astype(BF16).reshape(128, 2, 1024)
    whole = dot(pick_last, tok)
    halves = jnp.where(parity((256, 512), 0) == 0, whole[:, :512], whole[:, 512:])
    send[:, :, 1024:] = halves.astype(BF16).reshape(128, 2, 512)
    rows[y, me] = send[me]
    all_tokens[y] = tok
    shared_w[z, w, :, :128] = shared_gate[...]
    shared_w[z, w, :, 128:] = shared_up[...]

    with jax.named_scope("barrier"):
        pl.semaphore_wait(barrier, PEERS - 1 + 3)

    def inject(i):
        for k in range(0 if ORDER[i] else 1, PER_PLANE):
            peer = ep_peer(ORDER[i], k)
            remote(send.at[index_of(peer)], rows.at[y, me], send_sem, row_sem.at[i], peer).start()

    def ring(h, side):
        plane = (z + PLANES - (h - 1)) % PLANES if side == 0 else (z + h - 1) % PLANES
        block = shared_w.at[plane, w]
        peer = ep_peer(1 if side == 0 else PLANES - 1, 0)
        return remote(block, block, ring_send, ring_sem.at[side, h - 1], peer)

    def spread(plane):
        block = shared_w.at[plane, w]
        for n in (1, 2, 3):
            remote(block, block, wx_send, wx_sem.at[n - 1], ep_peer(0, 2 * n)).start()
        remote(block, block, wc_send, wc_sem.at[0], ep_peer(0, 1)).start()

    def ring_step(h):
        for side in (0, 1):
            if h > 1:
                ring(h - 1, side).wait_recv()
            if h <= NEAR:
                ring(h, side).start()
        if h == 1:
            spread(z)
        else:
            for plane in ((z + PLANES - (h - 1)) % PLANES, (z + h - 1) % PLANES):
                spread(plane)

    def jump():
        for far, first, last in ((NEAR, PLANES - NEAR, PLANES - 1), (PLANES - NEAR, 1, NEAR - 1)):
            for dz in range(first, last + 1):
                block = shared_w.at[(z + dz) % PLANES, w]
                remote(block, block, ring_send, jump_sem, ep_peer(far, 0)).start()

    def land():
        drain(shared_w.at[pl.ds(0, 2 * NEAR - 1), 0], jump_sem)
        for dz in range(NEAR + 1, PLANES - NEAR):
            spread((z + dz) % PLANES)

    def plane_of(i):
        return (z + PLANES - ORDER[i]) % PLANES

    def forward(i):
        group = rows.at[y, pl.ds(plane_of(i) * PER_PLANE, PER_PLANE)]
        if ORDER[i] == 0:
            drain(rows.at[y, pl.ds(0, PER_PLANE - 1)], row_sem.at[i])
        else:
            drain(group, row_sem.at[i])
        for n, d in enumerate((1, 3) if i < RELAYED else (1, 3, 2)):
            remote(group, group, fwd_send, fwd_sem.at[n, i], tp_peer(d)).start()

    def relay(i):
        at = plane_of(i) * PER_PLANE
        for n, d in enumerate((1, 3)):
            source = (y + 4 - d) % 4
            drain(rows.at[source, pl.ds(at, PER_PLANE)], fwd_sem.at[n, i])
            half = rows.at[source, pl.ds(at + 4 * n, 4)]
            remote(half, half, fwd_send, fwd_sem.at[2 + n, i], tp_peer(d)).start()

    even = parity((64, 512), 0) == 0

    def gain_row(t):
        return jnp.concatenate([gain[8 * t + n : 8 * t + n + 1, :] for n in range(8)], axis=1)

    def expert_in(b):
        for i in range(4 * b, 4 * b + 4):
            for n in (2, 3) if i < RELAYED else (0, 1, 2):
                drain(rows.at[0, pl.ds(0, 4 if i < RELAYED else PER_PLANE)], fwd_sem.at[n, i])

        def batch(t):
            parts = [
                rows[t, pl.ds(plane_of(i) * PER_PLANE, PER_PLANE)].reshape(16, 1536)
                for i in range(4 * b, 4 * b + 4)
            ]
            return jnp.concatenate(parts, axis=0)

        square_pair, square_last = jnp.zeros((64, 1), F32), jnp.zeros((64, 1), F32)
        for t in range(4):
            v = batch(t).astype(F32)
            sq = v * v
            square_pair += jnp.sum(sq[:, :1024], axis=1, keepdims=True)
            square_last += jnp.sum(sq[:, 1024:], axis=1, keepdims=True)
        last_wide = jnp.broadcast_to(square_last, (64, 128))
        square_last = (last_wide + swap_pairs(last_wide))[:, :1]
        scale_pair = lax.rsqrt(square_pair / 4096.0 + 1e-06)
        scale_last = lax.rsqrt(square_last / 4096.0 + 1e-06)
        for t in range(4):
            v = batch(t).astype(F32)
            g = gain_row(t)
            mixed_in[0:64, t * 1024 : (t + 1) * 1024] = (v[:, :1024] * scale_pair * g).astype(BF16)
            last = v[:, 1024:] * scale_last
            for p in (0, 1):
                mine = even if p == 0 else jnp.logical_not(even)
                part = jnp.where(mine, last * g[:, p * 512 : (p + 1) * 512], 0.0)
                at = t * 1024 + p * 512
                mixed_in[64:128, at : at + 512] = part.astype(BF16)
        both = dot(mixed_in[...], gate_up[...])
        tail = both[64:]
        both = jnp.concatenate([both[:64], tail + swap_pairs(tail)], axis=0)
        hidden[y, b] = silu_mul(both[:, :128], both[:, 128:]).astype(BF16)
        for n, d in enumerate(tps):
            remote(hidden.at[y, b], hidden.at[y, b], hid_send, hid_sem.at[n, b], tp_peer(d)).start()

    def expert_out(b):
        for n in range(3):
            drain(hidden.at[0, 0], hid_sem.at[n, b])
        full = jnp.concatenate([hidden[t, b] for t in range(4)], axis=1)
        res = dot(full, down[...])
        tail = jnp.where(even, res[64:, :512], res[64:, 512:])
        res = jnp.concatenate([res[:64], tail], axis=1).astype(BF16)
        for j in range(4):
            i = 4 * b + j
            plane = plane_of(i)
            give[pl.ds(plane * PER_PLANE, PER_PLANE)] = res[16 * j : 16 * j + 16].reshape(8, 2, 1536)
            for k in range(0 if ORDER[i] else 1, PER_PLANE):
                peer = ep_peer((PLANES - ORDER[i]) % PLANES, k)
                remote(give.at[index_of(peer)], got.at[me], give_send, got_sem, peer).start()
            if ORDER[i] == 0:
                got[me] = give[me]

    def columns(dx):
        return shared_w.at[:, ((x + 4 - dx) % 4) * 2 + c]

    def other_core(dx):
        return remote(columns(dx), columns(dx), wc_send, wc_sem.at[dx], ep_peer(0, 1))

    def pass_columns():
        for n in (1, 2, 3):
            drain(shared_w.at[:, 0], wx_sem.at[n - 1])
            other_core(n).start()

    def send_tokens():
        for n, d in enumerate(tps):
            remote(all_tokens.at[y], all_tokens.at[y], tok_send, tok_sem.at[n], tp_peer(d)).start()

    def shared_norm():
        for n in range(3):
            drain(all_tokens.at[0], tok_sem.at[n])
        square = jnp.zeros((128, 1), F32)
        for t in range(4):
            v = all_tokens[t].astype(F32)
            square += jnp.sum(v * v, axis=1, keepdims=True)
        scale = lax.rsqrt(square / 4096.0 + 1e-06)
        for t in range(4):
            v = all_tokens[t].astype(F32)
            normed[:, t * 1024 : (t + 1) * 1024] = (v * scale * gain_row(t)).astype(BF16)

    def shared_in():
        for n in range(4):
            drain(shared_w.at[:, 0], wc_sem.at[n])
        both = dot(normed[...], shared_w[...].reshape(4096, 256))
        shared_hidden[y] = silu_mul(both[:, :128], both[:, 128:]).astype(BF16)
        for n, d in enumerate(tps):
            remote(shared_hidden.at[y], shared_hidden.at[y], sh_send, sh_sem.at[n], tp_peer(d)).start()

    loaded = False
    injected, relayed = 0, 0
    for step in SCHEDULE:
        what, n = step[0], int(step[1:])
        with jax.named_scope(step):
            if what == "R":
                ring_step(n)
            elif what == "I":
                while injected < n:
                    inject(injected)
                    injected += 1
            elif what == "F":
                forward(n)
                while relayed <= min(n - LAG, RELAYED - 1):
                    relay(relayed)
                    relayed += 1
            elif what == "E":
                while relayed < min(4 * n + 4, RELAYED):
                    relay(relayed)
                    relayed += 1
                if not loaded:
                    for load in loads:
                        load.wait()
                    loaded = True
                expert_in(n)
            elif what == "D":
                expert_out(n)
            elif what == "T":
                send_tokens()
            elif what == "J":
                ring_step(NEAR + 1)
                jump()
            elif what == "K":
                land()
            elif what == "X":
                pass_columns()
            elif what == "S":
                (shared_norm, shared_in)[n]()

    token = expert

    def column(v):
        return jnp.sum(jnp.where(token == lane, v, jnp.zeros_like(v)), axis=1, keepdims=True)

    first, second = column(ids_t[0:1, :]), column(ids_t[1:2, :])
    gate0, gate1 = column(gates_t[0:1, :]), column(gates_t[1:2, :])
    names0, names1 = (lane == first).astype(F32), (lane == second).astype(F32)
    before = dot((lane < token).astype(BF16), (names0 + names1).astype(BF16))
    slot0 = jnp.sum(names0 * before, axis=1, keepdims=True).astype(jnp.int32)
    slot1 = jnp.sum(names1 * before, axis=1, keepdims=True).astype(jnp.int32)
    col = lax.broadcasted_iota(jnp.int32, (128, 256), 1)

    def weights(at, key0, key1):
        return jnp.where(at == key0, gate0, 0.0) + jnp.where(at == key1, gate1, 0.0)

    def parts_of(v):
        high = v.astype(BF16)
        return high, (v - high.astype(F32)).astype(BF16)

    pair = weights(
        col, jnp.where(slot0 < 2, 2 * first + slot0, -1), jnp.where(slot1 < 2, 2 * second + slot1, -1)
    )
    last = weights(col // 2, jnp.where(slot0 == 2, first, -1), jnp.where(slot1 == 2, second, -1))

    with jax.named_scope("shwait"):
        for n in range(3):
            drain(shared_hidden.at[0], sh_sem.at[n])
    full = jnp.concatenate([shared_hidden[t] for t in range(4)], axis=1)
    shared_out = dot(full, shared_down[...])

    with jax.named_scope("gotwait"):
        drain(got.at[pl.ds(0, PEERS - 1)], got_sem)
    back = got[...].reshape(256, 1536)
    total = shared_out
    for part in parts_of(pair):
        total += dot(part, back[:, :1024])
    sides = []
    for p in (0, 1):
        side = jnp.zeros((128, 512), F32)
        for part in parts_of(jnp.where(col % 2 == p, last, 0.0)):
            side += dot(part, back[:, 1024:])
        sides.append(side)
    out[...] = (total + jnp.concatenate(sides, axis=1)).astype(BF16)

    drain(send.at[pl.ds(0, PEERS - 1)], send_sem)
    drain(rows.at[pl.ds(0, 3)], fwd_send)
    drain(hidden.at[pl.ds(0, 3)], hid_send)
    drain(give.at[pl.ds(0, PEERS - 1)], give_send)
    drain(all_tokens.at[pl.ds(0, 3)], tok_send)
    drain(shared_w.at[pl.ds(0, 15), 0], ring_send)
    drain(shared_w.at[:, pl.ds(0, 3)], wx_send)
    drain(shared_w.at[:, pl.ds(0, 4)], wc_send)
    drain(shared_hidden.at[pl.ds(0, 3)], sh_send)


def shards(
    tokens,
    norm_gain,
    expert_ids,
    expert_gates,
    gate_proj,
    up_proj,
    down_proj,
    shared_gate,
    shared_up,
    shared_down,
):
    vmem, hbm = pl.BlockSpec(memory_space=pltpu.VMEM), pl.BlockSpec(memory_space=pl.ANY)
    dma = pltpu.SemaphoreType.DMA
    return pl.pallas_call(
        layer_kernel,
        out_shape=jax.ShapeDtypeStruct(tokens.shape, BF16),
        in_specs=[vmem, vmem, vmem, vmem, hbm, hbm, hbm, vmem, vmem, hbm],
        out_specs=vmem,
        scratch_shapes=[
            pltpu.VMEM((128, 2, 1536), BF16),
            pltpu.VMEM((4, 128, 2, 1536), BF16),
            pltpu.VMEM((128, 4096), BF16),
            pltpu.VMEM((4, BATCHES, 128, 128), BF16),
            pltpu.VMEM((128, 2, 1536), BF16),
            pltpu.VMEM((128, 2, 1536), BF16),
            pltpu.VMEM((4, 128, 1024), BF16),
            pltpu.VMEM((16, 8, 32, 256), BF16),
            pltpu.VMEM((4, 128, 128), BF16),
            pltpu.VMEM((128, 4096), BF16),
            pltpu.VMEM((4096, 256), BF16),
            pltpu.VMEM((512, 1024), BF16),
            pltpu.VMEM((512, 1024), BF16),
            dma((4,)),
            dma,
            dma((16,)),
            dma,
            dma((4, 16)),
            dma,
            dma((3, BATCHES)),
            dma,
            dma,
            dma,
            dma((3,)),
            dma,
            dma((2, NEAR)),
            dma,
            dma,
            dma((3,)),
            dma,
            dma((4,)),
            dma,
            dma((3,)),
        ],
        compiler_params=pltpu.CompilerParams(
            collective_id=0, has_side_effects=True, vmem_limit_bytes=60 * 2**20
        ),
    )(
        tokens,
        norm_gain.reshape(32, 128),
        expert_ids.T,
        expert_gates.T,
        gate_proj,
        up_proj,
        down_proj,
        shared_gate,
        shared_up,
        shared_down,
    )


def solution(mesh):
    finer = Mesh(mesh.devices.reshape(16, 4, 2, mesh.shape["tp"]), (*EP, "tp"))
    in_specs = (
        P(EP, "tp"),
        P(),
        P(EP, None),
        P(EP, None),
        P(EP, None, "tp"),
        P(EP, None, "tp"),
        P(EP, None, "tp"),
        P(EP, "tp"),
        P(EP, "tp"),
        P(None, "tp"),
    )
    return jax.shard_map(
        shards, mesh=finer, in_specs=in_specs, out_specs=P(EP, "tp"), check_vma=False
    )
```

```python
import jax
import jax.numpy as jnp
from jax import lax
from jax.experimental import pallas as pl
from jax.experimental.pallas import tpu as pltpu
from jax.sharding import Mesh
from jax.sharding import PartitionSpec as P

EP = ("ep_0", "ep_1", "ep_2")
MESH = pl.DeviceIdType.MESH
BF16 = jnp.bfloat16
F32 = jnp.float32
PLANES, PER_PLANE, PEERS = 16, 8, 128
BATCHES = 4
NEAR = 4
LAG = 2
RELAYED = 0


ORDER = (0, 1, 15, 2, 14, 3, 13, 4, 12, 5, 11, 6, 10, 7, 9, 8)
SCHEDULE = (
    "R1", "I8", "F0", "F1", "F2", "F3", "R2", "I12", "F4", "F5", "F6", "F7",
    "R3", "I16", "E0", "F8", "F9", "D0", "F10", "F11", "R4", "E1", "F12", "F13",
    "D1", "F14", "F15", "J0", "E2", "E3", "D2", "T0", "D3", "K0", "X0", "S0",
    "S1",
)


def dot(a, b):
    return jnp.dot(a, b, preferred_element_type=F32)


def parity(shape, axis):
    return lax.broadcasted_iota(jnp.int32, shape, axis) % 2


def swap_pairs(v):
    n = v.shape[0]
    return jnp.where(
        parity(v.shape, 0) == 0, pltpu.roll(v, n - 1, 0), pltpu.roll(v, 1, 0)
    )


def silu_mul(g, u):
    return g / (1.0 + jnp.exp(-g)) * u


def layer_kernel(
    tokens,
    gain,
    ids_t,
    gates_t,
    gate_hbm,
    up_hbm,
    down_hbm,
    shared_gate,
    shared_up,
    shared_down_hbm,
    out,
    send,
    rows,
    mixed_in,
    hidden,
    give,
    got,
    all_tokens,
    shared_w,
    shared_hidden,
    normed,
    total,
    gate_up,
    down,
    shared_down,
    load_sem,
    send_sem,
    row_sem,
    fwd_send,
    fwd_sem,
    hid_send,
    hid_sem,
    give_send,
    got_sem,
    tok_send,
    tok_sem,
    ring_send,
    ring_sem,
    jump_sem,
    wx_send,
    wx_sem,
    wc_send,
    wc_sem,
    sh_send,
    sh_sem,
):
    z, x, c, y = (lax.axis_index(a) for a in (*EP, "tp"))
    w = x * 2 + c
    me = z * PER_PLANE + w
    tps = (1, 3, 2)

    def remote(src, dst, ssem, rsem, device):
        return pltpu.make_async_remote_copy(
            src_ref=src,
            dst_ref=dst,
            send_sem=ssem,
            recv_sem=rsem,
            device_id=device,
            device_id_type=MESH,
        )

    def drain(ref, sem):
        pltpu.make_async_copy(ref, ref, sem).wait()

    def ep_peer(dz, k):
        return (z + dz) % PLANES, (x + k // 2) % 4, (c + k % 2) % 2, y

    def tp_peer(d):
        return z, x, c, (y + d) % 4

    def index_of(device):
        return (device[0] * 4 + device[1]) * 2 + device[2]

    barrier = pltpu.get_barrier_semaphore()

    for dz in range(PLANES):
        for k in range(0 if dz else 1, PER_PLANE):
            pl.semaphore_signal(barrier, inc=1, device_id=ep_peer(dz, k), device_id_type=MESH)
    for d in tps:
        pl.semaphore_signal(barrier, inc=1, device_id=tp_peer(d), device_id_type=MESH)

    loads = [
        pltpu.make_async_copy(gate_hbm.at[0], gate_up.at[:, pl.ds(0, 128)], load_sem.at[0]),
        pltpu.make_async_copy(up_hbm.at[0], gate_up.at[:, pl.ds(128, 128)], load_sem.at[1]),
        pltpu.make_async_copy(down_hbm.at[0], down, load_sem.at[2]),
        pltpu.make_async_copy(shared_down_hbm, shared_down, load_sem.at[3]),
    ]
    for load in loads:
        load.start()

    tok = tokens[...]
    expert = lax.broadcasted_iota(jnp.int32, (128, 128), 0)
    lane = lax.broadcasted_iota(jnp.int32, (128, 128), 1)
    first_t, second_t = ids_t[0:1, :], ids_t[1:2, :]
    names0, names1 = (expert == first_t).astype(F32), (expert == second_t).astype(F32)
    before = dot((names0 + names1).astype(BF16), (expert < lane).astype(BF16))
    slot0 = jnp.sum(names0 * before, axis=0, keepdims=True).astype(jnp.int32)
    slot1 = jnp.sum(names1 * before, axis=0, keepdims=True).astype(jnp.int32)

    row = lax.broadcasted_iota(jnp.int32, (256, 128), 0)
    pair0 = jnp.where(slot0 < 2, 2 * first_t + slot0, -1)
    pair1 = jnp.where(slot1 < 2, 2 * second_t + slot1, -1)
    last0 = jnp.where(slot0 == 2, first_t, -1)
    last1 = jnp.where(slot1 == 2, second_t, -1)
    pick_pair = ((row == pair0) | (row == pair1)).astype(BF16)
    pick_last = ((row // 2 == last0) | (row // 2 == last1)).astype(BF16)
    send[:, :, :1024] = dot(pick_pair, tok).astype(BF16).reshape(128, 2, 1024)
    whole = dot(pick_last, tok)
    halves = jnp.where(parity((256, 512), 0) == 0, whole[:, :512], whole[:, 512:])
    send[:, :, 1024:] = halves.astype(BF16).reshape(128, 2, 512)
    rows[y, me] = send[me]
    all_tokens[y] = tok
    shared_w[z, w, :, :128] = shared_gate[...]
    shared_w[z, w, :, 128:] = shared_up[...]

    with jax.named_scope("barrier"):
        pl.semaphore_wait(barrier, PEERS - 1 + 3)

    def inject(i):
        for k in range(0 if ORDER[i] else 1, PER_PLANE):
            peer = ep_peer(ORDER[i], k)
            remote(send.at[index_of(peer)], rows.at[y, me], send_sem, row_sem.at[i], peer).start()

    def ring(h, side):
        plane = (z + PLANES - (h - 1)) % PLANES if side == 0 else (z + h - 1) % PLANES
        block = shared_w.at[plane, w]
        peer = ep_peer(1 if side == 0 else PLANES - 1, 0)
        return remote(block, block, ring_send, ring_sem.at[side, h - 1], peer)

    def spread(plane):
        block = shared_w.at[plane, w]
        for n in (1, 2, 3):
            remote(block, block, wx_send, wx_sem.at[n - 1], ep_peer(0, 2 * n)).start()
        remote(block, block, wc_send, wc_sem.at[0], ep_peer(0, 1)).start()

    def ring_step(h):
        for side in (0, 1):
            if h > 1:
                ring(h - 1, side).wait_recv()
            if h <= NEAR:
                ring(h, side).start()
        if h == 1:
            spread(z)
        else:
            for plane in ((z + PLANES - (h - 1)) % PLANES, (z + h - 1) % PLANES):
                spread(plane)

    def jump(n, moves):
        for far, dz in moves:
            block = shared_w.at[(z + dz) % PLANES, w]
            remote(block, block, ring_send, jump_sem.at[n], ep_peer(far, 0)).start()

    def land(n, planes):
        drain(shared_w.at[pl.ds(0, len(planes)), 0], jump_sem.at[n])
        for dz in planes:
            spread((z + dz) % PLANES)

    def plane_of(i):
        return (z + PLANES - ORDER[i]) % PLANES

    def forward(i):
        group = rows.at[y, pl.ds(plane_of(i) * PER_PLANE, PER_PLANE)]
        if ORDER[i] == 0:
            drain(rows.at[y, pl.ds(0, PER_PLANE - 1)], row_sem.at[i])
        else:
            drain(group, row_sem.at[i])
        for n, d in enumerate((1, 3) if i < RELAYED else (1, 3, 2)):
            remote(group, group, fwd_send, fwd_sem.at[n, i], tp_peer(d)).start()

    def relay(i):
        at = plane_of(i) * PER_PLANE
        for n, d in enumerate((1, 3)):
            source = (y + 4 - d) % 4
            drain(rows.at[source, pl.ds(at, PER_PLANE)], fwd_sem.at[n, i])
            half = rows.at[source, pl.ds(at + 4 * n, 4)]
            remote(half, half, fwd_send, fwd_sem.at[2 + n, i], tp_peer(d)).start()

    even = parity((64, 512), 0) == 0

    def gain_row(t):
        return jnp.concatenate([gain[8 * t + n : 8 * t + n + 1, :] for n in range(8)], axis=1)

    def expert_in(b):
        for i in range(4 * b, 4 * b + 4):
            for n in (2, 3) if i < RELAYED else (0, 1, 2):
                drain(rows.at[0, pl.ds(0, 4 if i < RELAYED else PER_PLANE)], fwd_sem.at[n, i])

        def batch(t):
            parts = [
                rows[t, pl.ds(plane_of(i) * PER_PLANE, PER_PLANE)].reshape(16, 1536)
                for i in range(4 * b, 4 * b + 4)
            ]
            return jnp.concatenate(parts, axis=0)

        square_pair, square_last = jnp.zeros((64, 1), F32), jnp.zeros((64, 1), F32)
        for t in range(4):
            v = batch(t).astype(F32)
            sq = v * v
            square_pair += jnp.sum(sq[:, :1024], axis=1, keepdims=True)
            square_last += jnp.sum(sq[:, 1024:], axis=1, keepdims=True)
        last_wide = jnp.broadcast_to(square_last, (64, 128))
        square_last = (last_wide + swap_pairs(last_wide))[:, :1]
        scale_pair = lax.rsqrt(square_pair / 4096.0 + 1e-06)
        scale_last = lax.rsqrt(square_last / 4096.0 + 1e-06)
        for t in range(4):
            v = batch(t).astype(F32)
            g = gain_row(t)
            mixed_in[0:64, t * 1024 : (t + 1) * 1024] = (v[:, :1024] * scale_pair * g).astype(BF16)
            last = v[:, 1024:] * scale_last
            for p in (0, 1):
                mine = even if p == 0 else jnp.logical_not(even)
                part = jnp.where(mine, last * g[:, p * 512 : (p + 1) * 512], 0.0)
                at = t * 1024 + p * 512
                mixed_in[64:128, at : at + 512] = part.astype(BF16)
        both = dot(mixed_in[...], gate_up[...])
        tail = both[64:]
        both = jnp.concatenate([both[:64], tail + swap_pairs(tail)], axis=0)
        hidden[y, b] = silu_mul(both[:, :128], both[:, 128:]).astype(BF16)
        for n, d in enumerate(tps):
            remote(hidden.at[y, b], hidden.at[y, b], hid_send, hid_sem.at[n, b], tp_peer(d)).start()

    def expert_out(b):
        for n in range(3):
            drain(hidden.at[0, 0], hid_sem.at[n, b])
        full = jnp.concatenate([hidden[t, b] for t in range(4)], axis=1)
        res = dot(full, down[...])
        tail = jnp.where(even, res[64:, :512], res[64:, 512:])
        res = jnp.concatenate([res[:64], tail], axis=1).astype(BF16)
        for j in range(4):
            i = 4 * b + j
            plane = plane_of(i)
            give[pl.ds(plane * PER_PLANE, PER_PLANE)] = res[16 * j : 16 * j + 16].reshape(8, 2, 1536)
            for k in range(0 if ORDER[i] else 1, PER_PLANE):
                peer = ep_peer((PLANES - ORDER[i]) % PLANES, k)
                remote(give.at[index_of(peer)], got.at[me], give_send, got_sem.at[b], peer).start()
            if ORDER[i] == 0:
                got[me] = give[me]

    def columns(dx):
        return shared_w.at[:, ((x + 4 - dx) % 4) * 2 + c]

    def other_core(dx):
        return remote(columns(dx), columns(dx), wc_send, wc_sem.at[dx], ep_peer(0, 1))

    def pass_columns():
        for n in (1, 2, 3):
            drain(shared_w.at[:, 0], wx_sem.at[n - 1])
            other_core(n).start()

    def send_tokens():
        for n, d in enumerate(tps):
            remote(all_tokens.at[y], all_tokens.at[y], tok_send, tok_sem.at[n], tp_peer(d)).start()

    def shared_norm():
        for n in range(3):
            drain(all_tokens.at[0], tok_sem.at[n])
        square = jnp.zeros((128, 1), F32)
        for t in range(4):
            v = all_tokens[t].astype(F32)
            square += jnp.sum(v * v, axis=1, keepdims=True)
        scale = lax.rsqrt(square / 4096.0 + 1e-06)
        for t in range(4):
            v = all_tokens[t].astype(F32)
            normed[:, t * 1024 : (t + 1) * 1024] = (v * scale * gain_row(t)).astype(BF16)

    def shared_in():
        for n in range(4):
            drain(shared_w.at[:, 0], wc_sem.at[n])
        both = dot(normed[...], shared_w[...].reshape(4096, 256))
        shared_hidden[y] = silu_mul(both[:, :128], both[:, 128:]).astype(BF16)
        for n, d in enumerate(tps):
            remote(shared_hidden.at[y], shared_hidden.at[y], sh_send, sh_sem.at[n], tp_peer(d)).start()

    loaded = False
    injected, relayed = 0, 0
    for step in SCHEDULE:
        what, n = step[0], int(step[1:])
        with jax.named_scope(step):
            if what == "R":
                ring_step(n)
            elif what == "I":
                while injected < n:
                    inject(injected)
                    injected += 1
            elif what == "F":
                forward(n)
                while relayed <= min(n - LAG, RELAYED - 1):
                    relay(relayed)
                    relayed += 1
            elif what == "E":
                while relayed < min(4 * n + 4, RELAYED):
                    relay(relayed)
                    relayed += 1
                if not loaded:
                    for load in loads:
                        load.wait()
                    loaded = True
                expert_in(n)
            elif what == "D":
                expert_out(n)
            elif what == "T":
                send_tokens()
            elif what == "J":
                ring_step(NEAR + 1)
                jump(0, ((4, 12), (4, 13), (4, 14), (4, 15), (12, 1), (12, 2), (12, 3)))
            elif what == "K":
                land(0, (5, 6, 7, 8, 9, 10, 11))
            elif what == "X":
                pass_columns()
            elif what == "S":
                (shared_norm, shared_in)[n]()

    token = expert

    def column(v):
        return jnp.sum(jnp.where(token == lane, v, jnp.zeros_like(v)), axis=1, keepdims=True)

    first, second = column(ids_t[0:1, :]), column(ids_t[1:2, :])
    gate0, gate1 = column(gates_t[0:1, :]), column(gates_t[1:2, :])
    names0, names1 = (lane == first).astype(F32), (lane == second).astype(F32)
    before = dot((lane < token).astype(BF16), (names0 + names1).astype(BF16))
    slot0 = jnp.sum(names0 * before, axis=1, keepdims=True).astype(jnp.int32)
    slot1 = jnp.sum(names1 * before, axis=1, keepdims=True).astype(jnp.int32)
    col = lax.broadcasted_iota(jnp.int32, (128, 64), 1)
    pair0 = jnp.where(slot0 < 2, 2 * first + slot0, -1)
    pair1 = jnp.where(slot1 < 2, 2 * second + slot1, -1)
    last0 = jnp.where(slot0 == 2, first, -1)
    last1 = jnp.where(slot1 == 2, second, -1)

    def weights(at, key0, key1):
        return jnp.where(at == key0, gate0, 0.0) + jnp.where(at == key1, gate1, 0.0)

    def parts_of(v):
        high = v.astype(BF16)
        return high, (v - high.astype(F32)).astype(BF16)

    def combine(b):
        planes = [(z + ORDER[i]) % PLANES for i in range(4 * b, 4 * b + 4)]
        at = col % 16
        for j, plane in enumerate(planes):
            at = jnp.where(col // 16 == j, at + plane * 16, at)
        pair = parts_of(weights(at, pair0, pair1))
        last = weights(at // 2, last0, last1)
        sides = [parts_of(jnp.where(col % 2 == p, last, 0.0)) for p in (0, 1)]
        own = 0 in ORDER[4 * b : 4 * b + 4]
        drain(got.at[pl.ds(0, 4 * PER_PLANE - own)], got_sem.at[b])
        back = jnp.concatenate(
            [got[pl.ds(plane * PER_PLANE, PER_PLANE)].reshape(16, 1536) for plane in planes], axis=0
        )
        tail = back[:, 1024:]
        return dot(pair[0], back[:, :1024]) + dot(pair[1], back[:, :1024]) + jnp.concatenate(
            [dot(side[0], tail) + dot(side[1], tail) for side in sides], axis=1
        )

    with jax.named_scope("shwait"):
        for n in range(3):
            drain(shared_hidden.at[0], sh_sem.at[n])
    full = jnp.concatenate([shared_hidden[t] for t in range(4)], axis=1)
    total[...] = dot(full, shared_down[...])
    for b in range(BATCHES):
        with jax.named_scope(f"C{b}"):
            if b < BATCHES - 1:
                total[...] += combine(b)
            else:
                out[...] = (total[...] + combine(b)).astype(BF16)

    drain(send.at[pl.ds(0, PEERS - 1)], send_sem)
    drain(rows.at[pl.ds(0, 3)], fwd_send)
    drain(hidden.at[pl.ds(0, 3)], hid_send)
    drain(give.at[pl.ds(0, PEERS - 1)], give_send)
    drain(all_tokens.at[pl.ds(0, 3)], tok_send)
    drain(shared_w.at[pl.ds(0, 15), 0], ring_send)
    drain(shared_w.at[:, pl.ds(0, 3)], wx_send)
    drain(shared_w.at[:, pl.ds(0, 4)], wc_send)
    drain(shared_hidden.at[pl.ds(0, 3)], sh_send)


def shards(
    tokens,
    norm_gain,
    expert_ids,
    expert_gates,
    gate_proj,
    up_proj,
    down_proj,
    shared_gate,
    shared_up,
    shared_down,
):
    vmem, hbm = pl.BlockSpec(memory_space=pltpu.VMEM), pl.BlockSpec(memory_space=pl.ANY)
    dma = pltpu.SemaphoreType.DMA
    return pl.pallas_call(
        layer_kernel,
        out_shape=jax.ShapeDtypeStruct(tokens.shape, BF16),
        in_specs=[vmem, vmem, vmem, vmem, hbm, hbm, hbm, vmem, vmem, hbm],
        out_specs=vmem,
        scratch_shapes=[
            pltpu.VMEM((128, 2, 1536), BF16),
            pltpu.VMEM((4, 128, 2, 1536), BF16),
            pltpu.VMEM((128, 4096), BF16),
            pltpu.VMEM((4, BATCHES, 128, 128), BF16),
            pltpu.VMEM((128, 2, 1536), BF16),
            pltpu.VMEM((128, 2, 1536), BF16),
            pltpu.VMEM((4, 128, 1024), BF16),
            pltpu.VMEM((16, 8, 32, 256), BF16),
            pltpu.VMEM((4, 128, 128), BF16),
            pltpu.VMEM((128, 4096), BF16),
            pltpu.VMEM((128, 1024), F32),
            pltpu.VMEM((4096, 256), BF16),
            pltpu.VMEM((512, 1024), BF16),
            pltpu.VMEM((512, 1024), BF16),
            dma((4,)),
            dma,
            dma((16,)),
            dma,
            dma((4, 16)),
            dma,
            dma((3, BATCHES)),
            dma,
            dma((BATCHES,)),
            dma,
            dma((3,)),
            dma,
            dma((2, NEAR)),
            dma((2,)),
            dma,
            dma((3,)),
            dma,
            dma((4,)),
            dma,
            dma((3,)),
        ],
        compiler_params=pltpu.CompilerParams(
            collective_id=0, has_side_effects=True, vmem_limit_bytes=60 * 2**20
        ),
    )(
        tokens,
        norm_gain.reshape(32, 128),
        expert_ids.T,
        expert_gates.T,
        gate_proj,
        up_proj,
        down_proj,
        shared_gate,
        shared_up,
        shared_down,
    )


def solution(mesh):
    finer = Mesh(mesh.devices.reshape(16, 4, 2, mesh.shape["tp"]), (*EP, "tp"))
    in_specs = (
        P(EP, "tp"),
        P(),
        P(EP, None),
        P(EP, None),
        P(EP, None, "tp"),
        P(EP, None, "tp"),
        P(EP, None, "tp"),
        P(EP, "tp"),
        P(EP, "tp"),
        P(None, "tp"),
    )
    return jax.shard_map(
        shards, mesh=finer, in_specs=in_specs, out_specs=P(EP, "tp"), check_vma=False
    )
```
